32 devices in a mesh: sp: 8 (over z, y), dp: 4 (over x, core).
Axes of the slice: x: 2, y: 2, z: 4, core: 2. Of those that a mesh axis runs over, the one named last changes fastest.
Arguments:
- tokens: bfloat16 [4, 512, 1024], P('dp', 'sp'), may hold values from -6 to 6
- w_query: bfloat16 [1024, 512], P(None, ('sp', 'dp')), may hold values from -0.1875 to 0.1875
- w_forward: bfloat16 [1024, 512], P(None, ('sp', 'dp')), may hold values from -0.1875 to 0.1875
- w_backward: bfloat16 [1024, 512], P(None, ('sp', 'dp')), may hold values from -0.1875 to 0.1875
- w_input: bfloat16 [1024, 512], P(None, ('sp', 'dp')), may hold values from -0.1875 to 0.1875
- w_gate: bfloat16 [1024, 512], P(None, ('sp', 'dp')), may hold values from -0.1875 to 0.1875
- w_out: bfloat16 [512, 1024], P(None, ('sp', 'dp')), may hold values from -0.25 to 0.25
- memory_forward: float32 [512], replicated, may hold values from 0.3 to 4
- memory_backward: float32 [512], replicated, may hold values from 0.3 to 4
- norm_gain: float32 [128], replicated, may hold values from 0.1 to 1.9
Outputs:
- mixed: bfloat16 [4, 512, 1024], P('dp', 'sp')
The draws below stay inside these ranges and needn't reach their ends.
All inputs are finite; a program needn't handle non-finite values.
Results may differ from the reference program's by a relative error of at most 0.015.
Values may be sent and summed in bfloat16 or wider, within the bound.
A program may use at most 64 MiB of HBM per device.

```python
import math
import jax
import jax.numpy as jnp
from jax import lax

D = 1024
HEADS = 4
HEAD_DIM = 128
BLOCK = 64
LEN = 512
SEQS = 4
WIDTH = 512


def steps_of(stream_key, shape, pieces, low, top_value):
    loudness = 1.0
    for dim, parts in pieces:
        heights = jax.random.uniform(jax.random.fold_in(jax.random.fold_in(stream_key, 6), dim), (parts,), jnp.float32, low / len(pieces), top_value / len(pieces))
        loudness = loudness * jnp.repeat(jnp.exp(heights), shape[dim] // parts).reshape((-1,) + (1,) * (len(shape) - 1 - dim))
    return loudness


def gaussian(stream_key, extent, deviation, limit, pieces=(), kind=jnp.bfloat16):
    result = deviation * jax.random.normal(stream_key, extent, jnp.float32)
    if pieces:
        result = result * steps_of(stream_key, extent, pieces, -0.22, 0.18)
    return jnp.clip(result, -limit, limit).astype(kind)


def setup_inputs(seed: int = 0) -> dict:
    key_list = jax.random.split(jax.random.key(seed), 11)
    tokens = gaussian(key_list[0], (SEQS, LEN, D), 1.0, 6.0, ((0, 4), (1, 8)))
    w_query = gaussian(key_list[1], (D, WIDTH), D ** -0.5, 0.1875, ((1, 32),))
    w_forward = gaussian(key_list[2], (D, WIDTH), D ** -0.5, 0.1875, ((1, 32),))
    w_backward = gaussian(key_list[3], (D, WIDTH), D ** -0.5, 0.1875, ((1, 32),))
    w_input = gaussian(key_list[4], (D, WIDTH), D ** -0.5, 0.1875, ((1, 32),))
    w_gate = gaussian(key_list[5], (D, WIDTH), D ** -0.5, 0.1875, ((1, 32),))
    w_out = gaussian(key_list[6], (WIDTH, D), WIDTH ** -0.5, 0.25, ((1, 32),))
    memory_forward = jnp.clip(jnp.exp(jax.random.uniform(key_list[7], (WIDTH,), jnp.float32, math.log(0.3), math.log(4.0))), 0.3, 4.0)
    memory_backward = jnp.clip(jnp.exp(jax.random.uniform(key_list[8], (WIDTH,), jnp.float32, math.log(0.3), math.log(4.0))), 0.3, 4.0)
    norm_gain = jnp.clip(1.0 + 0.18 * jax.random.normal(key_list[9], (HEAD_DIM,), jnp.float32), 0.1, 1.9)
    return {"tokens": tokens, "w_query": w_query, "w_forward": w_forward, "w_backward": w_backward, "w_input": w_input, "w_gate": w_gate, "w_out": w_out, "memory_forward": memory_forward, "memory_backward": memory_backward, "norm_gain": norm_gain}


norm_eps = 1e-06
highest = lax.Precision.HIGHEST

def log_forget(projected, memory, seq_len):
    slack_value = memory / seq_len
    return jnp.logaddexp(jnp.log1p(-slack_value), jnp.log(slack_value) + jax.nn.log_sigmoid(projected.astype(jnp.float32)))

def sweep(queries, log_decay, values):
    seq_len, key_width = queries.shape
    blocks = seq_len // BLOCK
    input_keys = -jnp.expm1(log_decay)
    lower_mask = jnp.tril(jnp.ones((BLOCK, BLOCK), dtype=bool))[:, :, None]

    def advance(carry_state, inputs):
        query_part, decay_part, key_part, value_part = inputs
        running = jnp.cumsum(decay_part, axis=0)
        from_state = jnp.dot(query_part * jnp.exp(running), carry_state, precision=highest)
        gaps = running[:, None, :] - running[None, :, :]
        decay_table = jnp.where(lower_mask, jnp.exp(jnp.where(lower_mask, gaps, 0.0)), 0.0)
        scores = lax.optimization_barrier(jnp.sum(query_part[:, None, :] * key_part[None, :, :] * decay_table, axis=2))
        inside = jnp.dot(scores, value_part, precision=highest)
        final_sum = running[-1]
        weighted = key_part * jnp.exp(final_sum[None, :] - running)
        carry_state = jnp.exp(final_sum)[:, None] * carry_state + jnp.dot(weighted.T, value_part, precision=highest)
        return (carry_state, from_state + inside)

    def blocked(array):
        return array.reshape(blocks, BLOCK, array.shape[1])
    zero_state = jnp.zeros((key_width, values.shape[1]), jnp.float32)
    _, readings = lax.scan(advance, zero_state, (blocked(queries), blocked(log_decay), blocked(input_keys), blocked(values)))
    return readings.reshape(seq_len, values.shape[1])

def both_ways(queries, log_ahead, log_behind, values):
    forward_read = sweep(queries, log_ahead, values)
    behind = sweep(jnp.flip(queries, 0), jnp.flip(log_behind, 0), jnp.flip(values, 0))
    return forward_read + jnp.flip(behind, 0)

def reference(tokens, w_query, w_forward, w_backward, w_input, w_gate, w_out, memory_forward, memory_backward, norm_gain):
    flat_tokens = tokens.reshape(SEQS * LEN, D)

    def project(weight):
        return jnp.dot(flat_tokens, weight, preferred_element_type=jnp.float32).astype(jnp.bfloat16)

    def per_head(array):
        return array.reshape(SEQS, LEN, HEADS, HEAD_DIM).transpose(0, 2, 1, 3)
    queries = per_head(jax.nn.silu(project(w_query).astype(jnp.float32)))
    log_ahead = per_head(log_forget(project(w_forward), memory_forward, LEN))
    log_behind = per_head(log_forget(project(w_backward), memory_backward, LEN))
    values = per_head(project(w_input).astype(jnp.float32))
    gate_rows = project(w_gate)
    readout = jax.vmap(jax.vmap(both_ways))(queries, log_ahead, log_behind, values)
    readout = lax.optimization_barrier(readout.astype(jnp.bfloat16)).astype(jnp.float32)
    normed = readout * lax.rsqrt(lax.optimization_barrier(jnp.mean(readout * readout, axis=-1, keepdims=True)) + norm_eps) * norm_gain
    normed = normed.transpose(0, 2, 1, 3).reshape(SEQS * LEN, WIDTH)
    gated_rows = (normed * jax.nn.silu(gate_rows.astype(jnp.float32))).astype(jnp.bfloat16)
    mixed_rows = jnp.dot(gated_rows, w_out, preferred_element_type=jnp.float32).astype(jnp.bfloat16)
    return mixed_rows.reshape(SEQS, LEN, D)
```

```python
import functools

import jax
import jax.numpy as jnp
from jax import lax
from jax.experimental import pallas as pl
from jax.experimental.pallas import tpu as pltpu
from jax.sharding import PartitionSpec as P

HEADS = 4
HEAD_DIM = 128
BLOCK = 64


norm_eps = 1e-06
highest = lax.Precision.HIGHEST


def as_sent(array):
    return jax.tree.map(lambda a: a.astype(jnp.bfloat16) if a.dtype == jnp.float32 else a, array)


def gathered_then(share, axis, dim, apply):
    everything = lax.all_gather(share, axis, axis=dim, tiled=True)
    return apply(everything, jnp.int32(0))


def log_forget(projected, memory, seq_len):
    slack_value = memory / seq_len
    return jnp.logaddexp(
        jnp.log1p(-slack_value),
        jnp.log(slack_value) + jax.nn.log_sigmoid(projected.astype(jnp.float32)),
    )


def sweep(queries, log_decay, values):
    seq_len, key_width = queries.shape
    blocks = seq_len // BLOCK
    input_keys = -jnp.expm1(log_decay)
    lower_mask = jnp.tril(jnp.ones((BLOCK, BLOCK), dtype=bool))[:, :, None]

    def advance(carry_state, inputs):
        query_part, decay_part, key_part, value_part = inputs
        running = jnp.cumsum(decay_part, axis=0)
        from_state = jnp.dot(query_part * jnp.exp(running), carry_state, precision=highest)
        gaps = running[:, None, :] - running[None, :, :]
        decay_table = jnp.where(lower_mask, jnp.exp(jnp.where(lower_mask, gaps, 0.0)), 0.0)
        scores = jnp.sum(query_part[:, None, :] * key_part[None, :, :] * decay_table, axis=2)
        inside = jnp.dot(scores, value_part, precision=highest)
        final_sum = running[-1]
        weighted = key_part * jnp.exp(final_sum[None, :] - running)
        carry_state = jnp.exp(final_sum)[:, None] * carry_state + jnp.dot(
            weighted.T, value_part, precision=highest
        )
        return (carry_state, from_state + inside)

    def blocked(array):
        return array.reshape(blocks, BLOCK, array.shape[1])

    zero_state = jnp.zeros((key_width, values.shape[1]), jnp.float32)
    _, readings = lax.scan(
        advance,
        zero_state,
        (blocked(queries), blocked(log_decay), blocked(input_keys), blocked(values)),
    )
    return readings.reshape(seq_len, values.shape[1])


def both_ways(queries, log_ahead, log_behind, values):
    forward_read = sweep(queries, log_ahead, values)
    behind = sweep(jnp.flip(queries, 0), jnp.flip(log_behind, 0), jnp.flip(values, 0))
    return forward_read + jnp.flip(behind, 0)


def body(
    tokens,
    w_query,
    w_forward,
    w_backward,
    w_input,
    w_gate,
    w_out,
    memory_forward,
    memory_backward,
    norm_gain,
):
    seq_count, tok_count, model_width = tokens.shape
    row_count = seq_count * tok_count
    flat_tokens = tokens.reshape(row_count, model_width)
    group_count = lax.axis_size("sp")
    per_head_groups = group_count // HEADS
    block_width = HEAD_DIM // per_head_groups
    head_index = lax.axis_index("sp") // per_head_groups
    full_query, full_forward, full_backward, full_input, full_gate = (
        lax.all_gather(w_query, ("sp", "dp"), axis=1, tiled=True),
        lax.all_gather(w_forward, ("sp", "dp"), axis=1, tiled=True),
        lax.all_gather(w_backward, ("sp", "dp"), axis=1, tiled=True),
        lax.all_gather(w_input, ("sp", "dp"), axis=1, tiled=True),
        lax.all_gather(w_gate, ("sp", "dp"), axis=1, tiled=True),
    )

    def project(weight):
        return jnp.dot(flat_tokens, weight, preferred_element_type=jnp.float32).astype(jnp.bfloat16)

    def by_head(projected):
        shaped = projected.reshape(row_count, HEADS, 1, HEAD_DIM)
        spread_out = jnp.broadcast_to(shaped, (row_count, HEADS, per_head_groups, HEAD_DIM))
        return spread_out.reshape(row_count, group_count, HEAD_DIM)

    def by_group(projected):
        return projected.reshape(row_count, group_count, block_width)

    query_heads, ahead_heads, behind_heads, value_heads = (
        lax.all_to_all(
            as_sent(by_head(project(full_query))), "sp", split_axis=1, concat_axis=0, tiled=True
        ),
        lax.all_to_all(
            as_sent(by_head(project(full_forward))), "sp", split_axis=1, concat_axis=0, tiled=True
        ),
        lax.all_to_all(
            as_sent(by_head(project(full_backward))), "sp", split_axis=1, concat_axis=0, tiled=True
        ),
        lax.all_to_all(
            as_sent(by_group(project(full_input))), "sp", split_axis=1, concat_axis=0, tiled=True
        ),
    )
    gate_rows = project(full_gate)
    seq_len = query_heads.shape[0]
    memory_ahead = lax.dynamic_slice_in_dim(memory_forward, head_index * HEAD_DIM, HEAD_DIM)
    memory_behind = lax.dynamic_slice_in_dim(memory_backward, head_index * HEAD_DIM, HEAD_DIM)
    queries = jax.nn.silu(query_heads[:, 0].astype(jnp.float32))
    log_ahead = log_forget(ahead_heads[:, 0], memory_ahead, seq_len)
    log_behind = log_forget(behind_heads[:, 0], memory_behind, seq_len)
    values = value_heads[:, 0].astype(jnp.float32)
    readout = both_ways(queries, log_ahead, log_behind, values).astype(jnp.bfloat16)
    returned = lax.all_to_all(
        readout.reshape(seq_len, 1, block_width), "sp", split_axis=0, concat_axis=1, tiled=True
    )
    readout_rows = returned.reshape(row_count, HEADS, HEAD_DIM).astype(jnp.float32)
    normed = (
        readout_rows
        * lax.rsqrt(jnp.mean(readout_rows * readout_rows, axis=-1, keepdims=True) + norm_eps)
        * norm_gain
    )
    normed = normed.reshape(row_count, HEADS * HEAD_DIM)
    gated_rows = (normed * jax.nn.silu(gate_rows.astype(jnp.float32))).astype(jnp.bfloat16)

    def output_block(weight_piece, first_index):
        return jnp.dot(gated_rows, weight_piece, preferred_element_type=jnp.float32).astype(
            jnp.bfloat16
        )

    mixed_rows = gathered_then(w_out, ("sp", "dp"), 1, output_block)
    return mixed_rows.reshape(seq_count, tok_count, model_width)


def dot_nt(left, right):
    return lax.dot_general(
        left, right, (((1,), (1,)), ((), ())), preferred_element_type=jnp.float32
    )


def layer_kernel(
    members,
    columns,
    tokens,
    w_query,
    w_forward,
    w_backward,
    w_input,
    w_gate,
    w_out,
    memory_forward,
    memory_backward,
    norm_gain,
    mixed,
    token_all,
    weight_all,
    out_all,
    raw,
    mixed_heads,
    gated_own,
    sum_mask,
    token_send,
    token_recv,
    weight_send,
    weight_recv,
    relay_send,
    relay_recv,
    out_send,
    out_recv,
    plane_send,
    plane_recv,
    back_send,
    back_recv,
    raw_send,
    raw_recv,
    gated_send,
    gated_recv,
    local_sem,
):
    bf16, f32 = jnp.bfloat16, jnp.float32
    block = tokens.shape[0]
    own_rows = HEADS * block
    sp, dp = lax.axis_index("sp"), lax.axis_index("dp")
    head, member = sp // members, lax.rem(sp, members)
    column, core = dp // 2, lax.rem(dp, 2)
    seq_len = own_rows * members

    def turned(index, step, size):
        return lax.rem(index + step, size)

    def device(h, r, x, c):
        return {"sp": h * members + r, "dp": x * 2 + c}

    plane = [(a, b) for a in range(members) for b in range(columns) if (a, b) != (0, 0)]
    plane.sort(key=lambda ab: -((ab[0] != 0) + (ab[1] != 0)))

    def remote(src, dst, send, recv, where):
        return pltpu.make_async_remote_copy(
            src_ref=src,
            dst_ref=dst,
            send_sem=send,
            recv_sem=recv,
            device_id=where,
            device_id_type=pl.DeviceIdType.MESH,
        )

    across = [device(turned(head, k, HEADS), member, column, core) for k in range(1, HEADS)]
    beside = [
        device(head, turned(member, a, members), turned(column, b, columns), core)
        for a, b in plane
    ]
    partner = device(head, member, column, 1 - core)

    barrier = pltpu.get_barrier_semaphore()
    for where in across + beside + [partner]:
        pl.semaphore_signal(barrier, inc=1, device_id=where, device_id_type=pl.DeviceIdType.MESH)
    pl.semaphore_wait(barrier, len(across) + len(beside) + 1)

    weights = (w_query, w_forward, w_backward, w_input, w_gate)
    token_copies = []
    for k in range(1, HEADS):
        copy = remote(
            tokens,
            token_all.at[head],
            token_send.at[k - 1],
            token_recv.at[k - 1],
            across[k - 1],
        )
        copy.start()
        token_copies.append(copy)
    weight_copies = []
    for i, where in enumerate(beside + [partner]):
        for j, weight in enumerate(weights):
            copy = remote(
                weight,
                weight_all.at[j, member, dp],
                weight_send.at[i],
                weight_recv.at[i],
                where,
            )
            copy.start()
    out_copies = []
    for k in range(1, HEADS):
        copy = remote(
            w_out,
            out_all.at[head, member, dp],
            out_send.at[k - 1],
            out_recv.at[k - 1],
            across[k - 1],
        )
        copy.start()
        out_copies.append(copy)
    local = [
        pltpu.make_async_copy(tokens, token_all.at[head], local_sem.at[0]),
        pltpu.make_async_copy(w_out, out_all.at[head, member, dp], local_sem.at[1]),
    ]
    for j, weight in enumerate(weights):
        local.append(
            pltpu.make_async_copy(weight, weight_all.at[j, member, dp], local_sem.at[2 + j])
        )
    for copy in local:
        copy.start()

    def places(shape, dim, slot):
        row = lax.broadcasted_iota(jnp.int32, shape, dim)
        return (row // block) * (members * block) + lax.rem(row, block) + turned(
            member, slot, members
        ) * block

    for a in range(members):
        for b in range(members):
            shape = (own_rows, own_rows)
            earlier = places(shape, 1, b) <= places(shape, 0, a)
            sum_mask[a * own_rows : (a + 1) * own_rows, b * own_rows : (b + 1) * own_rows] = (
                jnp.where(earlier, 1.0, 0.0).astype(bf16)
            )

    for copy in local:
        copy.wait()

    def weight_block(r, x, c):
        return weight_all.at[:, r, x * 2 + c]

    relays = []
    for i, (a, b) in enumerate(plane):
        r = turned(member, members - a, members)
        x = turned(column, columns - b, columns)
        landed = weight_block(r, x, core)
        remote(landed, landed, weight_send.at[i], weight_recv.at[i], partner).wait_recv()
        copy = remote(landed, landed, relay_send.at[i], relay_recv.at[i], partner)
        copy.start()
        relays.append(copy)
    last = len(plane)
    landed = weight_block(member, column, 1 - core)
    remote(landed, landed, weight_send.at[last], weight_recv.at[last], partner).wait_recv()
    for copy in relays:
        copy.wait_recv()
    for copy in token_copies:
        copy.wait_recv()

    depth = tokens.shape[1]
    rows = token_all[...].reshape(own_rows, depth)

    def project(first, count):
        weight = weight_all[first : first + count].reshape(count * HEAD_DIM, depth)
        return dot_nt(rows, weight).astype(bf16)

    sent = project(1, 3)
    for j in range(3):
        raw[0, j] = sent[:, j * HEAD_DIM : (j + 1) * HEAD_DIM]
    raw_copies = []
    for a in range(1, members):
        copy = remote(
            raw.at[0],
            raw.at[members - a],
            raw_send.at[a - 1],
            raw_recv.at[a - 1],
            device(head, turned(member, a, members), column, core),
        )
        copy.start()
        raw_copies.append(copy)
    for copy in out_copies:
        copy.wait_recv()
    plane_copies = []
    mine = out_all.at[:, member, dp]
    for i, where in enumerate(beside + [partner]):
        copy = remote(mine, mine, plane_send.at[i], plane_recv.at[i], where)
        copy.start()
        plane_copies.append(copy)

    gate = project(4, 1).astype(f32)
    query = project(0, 1).astype(f32)
    queries = query * jax.nn.sigmoid(query)
    gate = gate * jax.nn.sigmoid(gate)

    for copy in raw_copies:
        copy.wait_recv()

    channels = pl.ds(pl.multiple_of(head * HEAD_DIM, HEAD_DIM), HEAD_DIM)

    def keys_of(j, memory):
        slack_value = memory[:, channels] / seq_len
        projected = raw[:, j].reshape(seq_len, HEAD_DIM).astype(f32)
        key = slack_value * jax.nn.sigmoid(-projected)
        return key, jnp.log1p(-key)

    key_ahead, log_ahead = keys_of(0, memory_forward)
    key_behind, log_behind = keys_of(1, memory_backward)
    values = raw[:, 2].reshape(seq_len, HEAD_DIM)
    logs = jnp.concatenate([log_ahead, log_behind], axis=1)
    coarse = logs.astype(bf16)
    fine = (logs - coarse.astype(f32)).astype(bf16)
    sums = jnp.dot(
        sum_mask[...], jnp.concatenate([coarse, fine], axis=1), preferred_element_type=f32
    )
    sums = sums[:, : 2 * HEAD_DIM] + sums[:, 2 * HEAD_DIM :]
    ahead = sums[:, :HEAD_DIM]
    behind = sums[:, HEAD_DIM:] - log_behind
    query_ahead = (queries * jnp.exp(ahead[:own_rows])).astype(bf16)
    query_behind = (queries * jnp.exp(-behind[:own_rows])).astype(bf16)
    key_ahead = (key_ahead * jnp.exp(-ahead)).astype(bf16)
    key_behind = (key_behind * jnp.exp(behind)).astype(bf16)

    readout = jnp.zeros((own_rows, HEAD_DIM), f32)
    for b in range(members):
        part = slice(b * own_rows, (b + 1) * own_rows)
        shape = (own_rows, own_rows)
        there, here = places(shape, 1, b), places(shape, 0, 0)
        scores = jnp.where(there <= here, dot_nt(query_ahead, key_ahead[part]), 0.0) + jnp.where(
            there >= here, dot_nt(query_behind, key_behind[part]), 0.0
        )
        readout = readout + jnp.dot(
            scores.astype(bf16), values[part], preferred_element_type=f32
        )
    readout = readout.astype(bf16).astype(f32)
    square = jnp.mean(readout * readout, axis=-1, keepdims=True)
    gated = (readout * lax.rsqrt(square + norm_eps) * norm_gain[...] * gate).astype(bf16)
    gated_own[...] = gated.reshape(HEADS, block, HEAD_DIM)

    gated_copies = []
    for k in range(1, HEADS):
        copy = remote(
            gated_own.at[turned(head, k, HEADS)],
            mixed_heads.at[head],
            gated_send.at[k - 1],
            gated_recv.at[k - 1],
            across[k - 1],
        )
        copy.start()
        gated_copies.append(copy)
    own = pltpu.make_async_copy(gated_own.at[head], mixed_heads.at[head], local_sem.at[0])
    own.start()

    back_copies = []
    for i, (a, b) in enumerate(plane):
        r = turned(member, members - a, members)
        x = turned(column, columns - b, columns)
        plane_copies[i].wait_recv()
        landed = out_all.at[:, r, x * 2 + core]
        copy = remote(landed, landed, back_send.at[i], back_recv.at[i], partner)
        copy.start()
        back_copies.append(copy)
    plane_copies[last].wait_recv()
    for copy in back_copies:
        copy.wait_recv()
    own.wait()
    for copy in gated_copies:
        copy.wait_recv()

    total = jnp.zeros((block, depth), f32)
    weight = out_all[...].reshape(depth, HEADS * HEAD_DIM)
    joined = jnp.concatenate([mixed_heads[h] for h in range(HEADS)], axis=1)
    mixed[...] = dot_nt(joined, weight).astype(bf16)

    for copy in token_copies + relays + out_copies + plane_copies + back_copies:
        copy.wait_send()
    for copy in raw_copies + gated_copies:
        copy.wait_send()
    mine = weight_block(member, column, core)
    for i in range(last + 1):
        remote(mine, mine, weight_send.at[i], weight_recv.at[i], partner).wait_send()


def whole_layer(
    members,
    columns,
    tokens,
    w_query,
    w_forward,
    w_backward,
    w_input,
    w_gate,
    w_out,
    memory_forward,
    memory_backward,
    norm_gain,
):
    _, block, depth = tokens.shape
    width = w_query.shape[1]
    out_width = w_out.shape[1]
    own_rows = HEADS * block
    seq_len = own_rows * members
    others = HEADS - 1
    beside = members * columns
    bf16 = jnp.bfloat16
    dma = pltpu.SemaphoreType.DMA
    vmem = pl.BlockSpec(memory_space=pltpu.VMEM)
    flat = pl.pallas_call(
        functools.partial(layer_kernel, members, columns),
        out_shape=jax.ShapeDtypeStruct((block, depth), bf16),
        in_specs=[vmem] * 10,
        out_specs=vmem,
        scratch_shapes=[
            pltpu.VMEM((HEADS, block, depth), bf16),
            pltpu.VMEM((5, members, 2 * columns, width, depth), bf16),
            pltpu.VMEM((HEADS, members, 2 * columns, out_width, HEADS * HEAD_DIM), bf16),
            pltpu.VMEM((members, 3, own_rows, HEAD_DIM), bf16),
            pltpu.VMEM((HEADS, block, HEAD_DIM), bf16),
            pltpu.VMEM((HEADS, block, HEAD_DIM), bf16),
            pltpu.VMEM((seq_len, seq_len), bf16),
            dma((others,)),
            dma((others,)),
            dma((beside,)),
            dma((beside,)),
            dma((beside,)),
            dma((beside,)),
            dma((others,)),
            dma((others,)),
            dma((beside,)),
            dma((beside,)),
            dma((beside,)),
            dma((beside,)),
            dma((members,)),
            dma((members,)),
            dma((others,)),
            dma((others,)),
            dma((7,)),
        ],
        compiler_params=pltpu.CompilerParams(
            collective_id=0, has_side_effects=True, vmem_limit_bytes=48 * 1024 * 1024
        ),
    )(
        tokens.reshape(block, depth),
        w_query.T,
        w_forward.T,
        w_backward.T,
        w_input.T,
        w_gate.T,
        w_out.T,
        memory_forward.reshape(1, -1),
        memory_backward.reshape(1, -1),
        norm_gain.reshape(1, -1),
    )
    return flat.reshape(1, block, depth)


def layer(mesh, tokens, w_query, *rest):
    members = mesh.shape["sp"] // HEADS
    columns = mesh.shape["dp"] // 2
    if tokens.shape[0] == 1 and w_query.shape[1] % 16 == 0:
        return whole_layer(members, columns, tokens, w_query, *rest)
    return body(tokens, w_query, *rest)


def solution(mesh):
    return jax.shard_map(
        functools.partial(layer, mesh),
        mesh=mesh,
        in_specs=(
            P("dp", "sp", None),
            P(None, ("sp", "dp")),
            P(None, ("sp", "dp")),
            P(None, ("sp", "dp")),
            P(None, ("sp", "dp")),
            P(None, ("sp", "dp")),
            P(None, ("sp", "dp")),
            P(),
            P(),
            P(),
        ),
        out_specs=P("dp", "sp", None),
        check_vma=False,
    )
```

```python
import functools

import jax
import jax.numpy as jnp
from jax import lax
from jax.experimental import pallas as pl
from jax.experimental.pallas import tpu as pltpu
from jax.sharding import PartitionSpec as P

HEADS = 4
HEAD_DIM = 128
BLOCK = 64


norm_eps = 1e-06
highest = lax.Precision.HIGHEST


def as_sent(array):
    return jax.tree.map(lambda a: a.astype(jnp.bfloat16) if a.dtype == jnp.float32 else a, array)


def gathered_then(share, axis, dim, apply):
    everything = lax.all_gather(share, axis, axis=dim, tiled=True)
    return apply(everything, jnp.int32(0))


def log_forget(projected, memory, seq_len):
    slack_value = memory / seq_len
    return jnp.logaddexp(
        jnp.log1p(-slack_value),
        jnp.log(slack_value) + jax.nn.log_sigmoid(projected.astype(jnp.float32)),
    )


def sweep(queries, log_decay, values):
    seq_len, key_width = queries.shape
    blocks = seq_len // BLOCK
    input_keys = -jnp.expm1(log_decay)
    lower_mask = jnp.tril(jnp.ones((BLOCK, BLOCK), dtype=bool))[:, :, None]

    def advance(carry_state, inputs):
        query_part, decay_part, key_part, value_part = inputs
        running = jnp.cumsum(decay_part, axis=0)
        from_state = jnp.dot(query_part * jnp.exp(running), carry_state, precision=highest)
        gaps = running[:, None, :] - running[None, :, :]
        decay_table = jnp.where(lower_mask, jnp.exp(jnp.where(lower_mask, gaps, 0.0)), 0.0)
        scores = jnp.sum(query_part[:, None, :] * key_part[None, :, :] * decay_table, axis=2)
        inside = jnp.dot(scores, value_part, precision=highest)
        final_sum = running[-1]
        weighted = key_part * jnp.exp(final_sum[None, :] - running)
        carry_state = jnp.exp(final_sum)[:, None] * carry_state + jnp.dot(
            weighted.T, value_part, precision=highest
        )
        return (carry_state, from_state + inside)

    def blocked(array):
        return array.reshape(blocks, BLOCK, array.shape[1])

    zero_state = jnp.zeros((key_width, values.shape[1]), jnp.float32)
    _, readings = lax.scan(
        advance,
        zero_state,
        (blocked(queries), blocked(log_decay), blocked(input_keys), blocked(values)),
    )
    return readings.reshape(seq_len, values.shape[1])


def both_ways(queries, log_ahead, log_behind, values):
    forward_read = sweep(queries, log_ahead, values)
    behind = sweep(jnp.flip(queries, 0), jnp.flip(log_behind, 0), jnp.flip(values, 0))
    return forward_read + jnp.flip(behind, 0)


def body(
    tokens,
    w_query,
    w_forward,
    w_backward,
    w_input,
    w_gate,
    w_out,
    memory_forward,
    memory_backward,
    norm_gain,
):
    seq_count, tok_count, model_width = tokens.shape
    row_count = seq_count * tok_count
    flat_tokens = tokens.reshape(row_count, model_width)
    group_count = lax.axis_size("sp")
    per_head_groups = group_count // HEADS
    block_width = HEAD_DIM // per_head_groups
    head_index = lax.axis_index("sp") // per_head_groups
    full_query, full_forward, full_backward, full_input, full_gate = (
        lax.all_gather(w_query, ("sp", "dp"), axis=1, tiled=True),
        lax.all_gather(w_forward, ("sp", "dp"), axis=1, tiled=True),
        lax.all_gather(w_backward, ("sp", "dp"), axis=1, tiled=True),
        lax.all_gather(w_input, ("sp", "dp"), axis=1, tiled=True),
        lax.all_gather(w_gate, ("sp", "dp"), axis=1, tiled=True),
    )

    def project(weight):
        return jnp.dot(flat_tokens, weight, preferred_element_type=jnp.float32).astype(jnp.bfloat16)

    def by_head(projected):
        shaped = projected.reshape(row_count, HEADS, 1, HEAD_DIM)
        spread_out = jnp.broadcast_to(shaped, (row_count, HEADS, per_head_groups, HEAD_DIM))
        return spread_out.reshape(row_count, group_count, HEAD_DIM)

    def by_group(projected):
        return projected.reshape(row_count, group_count, block_width)

    query_heads, ahead_heads, behind_heads, value_heads = (
        lax.all_to_all(
            as_sent(by_head(project(full_query))), "sp", split_axis=1, concat_axis=0, tiled=True
        ),
        lax.all_to_all(
            as_sent(by_head(project(full_forward))), "sp", split_axis=1, concat_axis=0, tiled=True
        ),
        lax.all_to_all(
            as_sent(by_head(project(full_backward))), "sp", split_axis=1, concat_axis=0, tiled=True
        ),
        lax.all_to_all(
            as_sent(by_group(project(full_input))), "sp", split_axis=1, concat_axis=0, tiled=True
        ),
    )
    gate_rows = project(full_gate)
    seq_len = query_heads.shape[0]
    memory_ahead = lax.dynamic_slice_in_dim(memory_forward, head_index * HEAD_DIM, HEAD_DIM)
    memory_behind = lax.dynamic_slice_in_dim(memory_backward, head_index * HEAD_DIM, HEAD_DIM)
    queries = jax.nn.silu(query_heads[:, 0].astype(jnp.float32))
    log_ahead = log_forget(ahead_heads[:, 0], memory_ahead, seq_len)
    log_behind = log_forget(behind_heads[:, 0], memory_behind, seq_len)
    values = value_heads[:, 0].astype(jnp.float32)
    readout = both_ways(queries, log_ahead, log_behind, values).astype(jnp.bfloat16)
    returned = lax.all_to_all(
        readout.reshape(seq_len, 1, block_width), "sp", split_axis=0, concat_axis=1, tiled=True
    )
    readout_rows = returned.reshape(row_count, HEADS, HEAD_DIM).astype(jnp.float32)
    normed = (
        readout_rows
        * lax.rsqrt(jnp.mean(readout_rows * readout_rows, axis=-1, keepdims=True) + norm_eps)
        * norm_gain
    )
    normed = normed.reshape(row_count, HEADS * HEAD_DIM)
    gated_rows = (normed * jax.nn.silu(gate_rows.astype(jnp.float32))).astype(jnp.bfloat16)

    def output_block(weight_piece, first_index):
        return jnp.dot(gated_rows, weight_piece, preferred_element_type=jnp.float32).astype(
            jnp.bfloat16
        )

    mixed_rows = gathered_then(w_out, ("sp", "dp"), 1, output_block)
    return mixed_rows.reshape(seq_count, tok_count, model_width)


GROUPS = ((0, 1, 2), (3,))


def dot_nt(left, right):
    return lax.dot_general(
        left, right, (((1,), (1,)), ((), ())), preferred_element_type=jnp.float32
    )


def layer_kernel(
    members,
    columns,
    tokens,
    w_query,
    w_forward,
    w_backward,
    w_input,
    w_gate,
    w_out,
    memory_forward,
    memory_backward,
    norm_gain,
    mixed,
    small,
    gain,
    query_gate,
    token_all,
    weight_all,
    out_all,
    raw,
    mixed_heads,
    gated_own,
    sum_mask,
    token_send,
    token_recv,
    weight_send,
    weight_recv,
    relay_send,
    relay_recv,
    out_send,
    out_recv,
    plane_send,
    plane_recv,
    back_send,
    back_recv,
    raw_send,
    raw_recv,
    gated_send,
    gated_recv,
    local_sem,
):
    bf16, f32 = jnp.bfloat16, jnp.float32
    block, depth = tokens.shape
    half = block // 2
    own_rows = HEADS * block
    sp, dp = lax.axis_index("sp"), lax.axis_index("dp")
    head, member = sp // members, lax.rem(sp, members)
    column, core = dp // 2, lax.rem(dp, 2)
    seq_len = own_rows * members
    heads = (head, head + 1 - 2 * lax.rem(head, 2), lax.rem(head + 2, HEADS), HEADS - 1 - head)

    def turned(index, step, size):
        return lax.rem(index + step, size)

    def device(h, r, x, c):
        return {"sp": h * members + r, "dp": x * 2 + c}

    plane = [(a, b) for a in range(members) for b in range(columns) if (a, b) != (0, 0)]
    plane.sort(key=lambda ab: -((ab[0] != 0) + (ab[1] != 0)))
    last = len(plane)

    def remote(src, dst, send, recv, where):
        return pltpu.make_async_remote_copy(
            src_ref=src,
            dst_ref=dst,
            send_sem=send,
            recv_sem=recv,
            device_id=where,
            device_id_type=pl.DeviceIdType.MESH,
        )

    across = [device(heads[k], member, column, core) for k in range(HEADS)]
    beside = [
        device(head, turned(member, a, members), turned(column, b, columns), core)
        for a, b in plane
    ]
    partner = device(head, member, column, 1 - core)

    weights = (w_query, w_forward, w_backward, w_input, w_gate)
    local = []
    for j, weight in enumerate(weights):
        local.append(pltpu.make_async_copy(weight, weight_all.at[j, member, dp], local_sem.at[j]))
    local.append(pltpu.make_async_copy(tokens, token_all.at[0], local_sem.at[5]))
    local.append(
        pltpu.make_async_copy(w_out, out_all.at[head, member, dp], local_sem.at[6])
    )
    local.append(pltpu.make_async_copy(memory_forward, small.at[0:1], local_sem.at[7]))
    local.append(pltpu.make_async_copy(memory_backward, small.at[1:2], local_sem.at[8]))
    local.append(pltpu.make_async_copy(norm_gain, gain, local_sem.at[9]))
    for copy in [local[5]] + local[:5] + local[6:]:
        copy.start()

    barrier = pltpu.get_barrier_semaphore()
    greeted = across[1:] + beside + [partner]
    for where in greeted:
        pl.semaphore_signal(barrier, inc=1, device_id=where, device_id_type=pl.DeviceIdType.MESH)
    pl.semaphore_wait(barrier, len(greeted))

    token_copies = []
    local[5].wait()

    def rows_of(k, piece):
        return token_all.at[k, piece * half : (piece + 1) * half]

    def send_tokens(source, slot, where):
        for piece in range(2):
            at = 2 * (slot - 1) + piece
            copy = remote(
                rows_of(source, piece),
                rows_of(slot, piece),
                token_send.at[at],
                token_recv.at[at],
                where,
            )
            token_copies.append(copy)

    send_tokens(0, 1, across[1])
    send_tokens(0, 2, across[2])
    for copy in token_copies:
        copy.start()

    def weight_block(r, x, c):
        return weight_all.at[:, r, x * 2 + c]

    for copy in local[:5]:
        copy.wait()
    mine = weight_block(member, column, core)
    weight_copies = []
    for i, where in enumerate(beside + [partner]):
        copy = remote(mine, mine, weight_send.at[i], weight_recv.at[i], where)
        copy.start()
        weight_copies.append(copy)
    local[6].wait()
    out_mine = out_all.at[head, member, dp]
    out_copies = []
    for k in (1, 2):
        copy = remote(out_mine, out_mine, out_send.at[k - 1], out_recv.at[k - 1], across[k])
        copy.start()
        out_copies.append(copy)

    def places(shape, dim, slot):
        row = lax.broadcasted_iota(jnp.int32, shape, dim)
        return (row // block) * (members * block) + lax.rem(row, block) + turned(
            member, slot, members
        ) * block

    for a in range(members):
        for b in range(members):
            shape = (own_rows, own_rows)
            earlier = places(shape, 1, b) <= places(shape, 0, a)
            sum_mask[a * own_rows : (a + 1) * own_rows, b * own_rows : (b + 1) * own_rows] = (
                jnp.where(earlier, 1.0, 0.0).astype(bf16)
            )

    send_tokens(2, 3, across[1])
    for piece in range(2):
        token_copies[2 + piece].wait_recv()
        token_copies[4 + piece].start()

    relays = []
    for i, (a, b) in enumerate(plane):
        r = turned(member, members - a, members)
        x = turned(column, columns - b, columns)
        landed = weight_block(r, x, core)
        weight_copies[i].wait_recv()
        copy = remote(landed, landed, relay_send.at[i], relay_recv.at[i], partner)
        copy.start()
        relays.append(copy)
    out_copies[1].wait_recv()
    landed = out_all.at[heads[2], member, dp]
    out_copies.append(remote(landed, landed, out_send.at[2], out_recv.at[2], across[1]))
    out_copies[2].start()
    weight_copies[last].wait_recv()
    for copy in relays:
        copy.wait_recv()

    def project(slots, first, count):
        rows = token_all[slots[0] : slots[-1] + 1].reshape(len(slots) * block, depth)
        weight = weight_all[first : first + count].reshape(count * HEAD_DIM, depth)
        return dot_nt(rows, weight).astype(bf16)

    raw_copies = []
    for slots in GROUPS:
        for slot in slots:
            if slot in (1, 3):
                for piece in range(2):
                    token_copies[2 * (slot - 1) + piece].wait_recv()
        sent = project(slots, 1, 3)
        for n, slot in enumerate(slots):
            for j in range(3):
                raw[0, j, heads[slot]] = sent[
                    n * block : (n + 1) * block, j * HEAD_DIM : (j + 1) * HEAD_DIM
                ]
        for slot in slots:
            for a in range(1, members):
                at = (a - 1) * HEADS + slot
                copy = remote(
                    raw.at[0, :, heads[slot]],
                    raw.at[members - a, :, heads[slot]],
                    raw_send.at[at],
                    raw_recv.at[at],
                    device(head, turned(member, a, members), column, core),
                )
                copy.start()
                raw_copies.append(copy)
        query = project(slots, 0, 1)
        gate = project(slots, 4, 1)
        for n, slot in enumerate(slots):
            query_gate[0, heads[slot]] = query[n * block : (n + 1) * block]
            query_gate[1, heads[slot]] = gate[n * block : (n + 1) * block]

    out_copies[0].wait_recv()
    out_copies[2].wait_recv()
    plane_copies = []
    mine = out_all.at[:, member, dp]
    for i, where in enumerate(beside + [partner]):
        copy = remote(mine, mine, plane_send.at[i], plane_recv.at[i], where)
        copy.start()
        plane_copies.append(copy)

    gate = query_gate[1].reshape(own_rows, HEAD_DIM).astype(f32)
    query = query_gate[0].reshape(own_rows, HEAD_DIM).astype(f32)
    queries = query * jax.nn.sigmoid(query)
    gate = gate * jax.nn.sigmoid(gate)
    for copy in local[7:]:
        copy.wait()

    channels = pl.ds(pl.multiple_of(head * HEAD_DIM, HEAD_DIM), HEAD_DIM)

    def keys_of(a, j):
        slack_value = small[j : j + 1, channels] / seq_len
        projected = raw[a, j].reshape(own_rows, HEAD_DIM).astype(f32)
        key = slack_value * jax.nn.sigmoid(-projected)
        return key, jnp.log1p(-key)

    made = [(keys_of(0, 0), keys_of(0, 1))]
    for copy in raw_copies:
        copy.wait_recv()
    for a in range(1, members):
        made.append((keys_of(a, 0), keys_of(a, 1)))

    def joined(way, item):
        return jnp.concatenate([one[way][item] for one in made], axis=0)

    key_ahead, log_ahead = joined(0, 0), joined(0, 1)
    key_behind, log_behind = joined(1, 0), joined(1, 1)
    values = raw[:, 2].reshape(seq_len, HEAD_DIM)
    logs = jnp.concatenate([log_ahead, log_behind], axis=1)
    coarse = logs.astype(bf16)
    fine = (logs - coarse.astype(f32)).astype(bf16)
    sums = jnp.dot(
        sum_mask[...], jnp.concatenate([coarse, fine], axis=1), preferred_element_type=f32
    )
    sums = sums[:, : 2 * HEAD_DIM] + sums[:, 2 * HEAD_DIM :]
    ahead = sums[:, :HEAD_DIM]
    behind = sums[:, HEAD_DIM:] - log_behind
    query_ahead = (queries * jnp.exp(ahead[:own_rows])).astype(bf16)
    query_behind = (queries * jnp.exp(-behind[:own_rows])).astype(bf16)
    key_ahead = (key_ahead * jnp.exp(-ahead)).astype(bf16)
    key_behind = (key_behind * jnp.exp(behind)).astype(bf16)

    readout = jnp.zeros((own_rows, HEAD_DIM), f32)
    for b in range(members):
        part = slice(b * own_rows, (b + 1) * own_rows)
        shape = (own_rows, own_rows)
        there, here = places(shape, 1, b), places(shape, 0, 0)
        scores = jnp.where(there <= here, dot_nt(query_ahead, key_ahead[part]), 0.0) + jnp.where(
            there >= here, dot_nt(query_behind, key_behind[part]), 0.0
        )
        readout = readout + jnp.dot(
            scores.astype(bf16), values[part], preferred_element_type=f32
        )
    readout = readout.astype(bf16).astype(f32)
    square = jnp.mean(readout * readout, axis=-1, keepdims=True)
    gated = (readout * lax.rsqrt(square + norm_eps) * gain[...] * gate).astype(bf16)
    gated_own[...] = gated.reshape(HEADS, block, HEAD_DIM)

    gated_copies = []
    for k in range(1, HEADS):
        copy = remote(
            gated_own.at[heads[k]],
            mixed_heads.at[head],
            gated_send.at[k - 1],
            gated_recv.at[k - 1],
            across[k],
        )
        copy.start()
        gated_copies.append(copy)
    mixed_heads[head] = gated_own[head]

    back_copies = []
    for i, (a, b) in enumerate(plane):
        r = turned(member, members - a, members)
        x = turned(column, columns - b, columns)
        plane_copies[i].wait_recv()
        landed = out_all.at[:, r, x * 2 + core]
        copy = remote(landed, landed, back_send.at[i], back_recv.at[i], partner)
        copy.start()
        back_copies.append(copy)
    plane_copies[last].wait_recv()
    for copy in back_copies:
        copy.wait_recv()
    for copy in gated_copies:
        copy.wait_recv()

    weight = out_all[...].reshape(depth, HEADS * HEAD_DIM)
    row = jnp.concatenate([mixed_heads[h] for h in range(HEADS)], axis=1)
    mixed[...] = dot_nt(row, weight).astype(bf16)

    for copy in token_copies + weight_copies + relays + out_copies + plane_copies + back_copies:
        copy.wait_send()
    for copy in raw_copies + gated_copies:
        copy.wait_send()


def whole_layer(
    members,
    columns,
    tokens,
    w_query,
    w_forward,
    w_backward,
    w_input,
    w_gate,
    w_out,
    memory_forward,
    memory_backward,
    norm_gain,
):
    _, block, depth = tokens.shape
    width = w_query.shape[1]
    out_width = w_out.shape[1]
    own_rows = HEADS * block
    seq_len = own_rows * members
    others = HEADS - 1
    beside = members * columns
    bf16 = jnp.bfloat16
    dma = pltpu.SemaphoreType.DMA
    hbm = pl.BlockSpec(memory_space=pltpu.HBM)
    vmem = pl.BlockSpec(memory_space=pltpu.VMEM)
    flat = pl.pallas_call(
        functools.partial(layer_kernel, members, columns),
        out_shape=jax.ShapeDtypeStruct((block, depth), bf16),
        in_specs=[hbm] * 10,
        out_specs=vmem,
        scratch_shapes=[
            pltpu.VMEM((2, HEADS * HEAD_DIM), jnp.float32),
            pltpu.VMEM((1, HEAD_DIM), jnp.float32),
            pltpu.VMEM((2, HEADS, block, HEAD_DIM), bf16),
            pltpu.VMEM((HEADS, block, depth), bf16),
            pltpu.VMEM((5, members, 2 * columns, width, depth), bf16),
            pltpu.VMEM((HEADS, members, 2 * columns, out_width, HEADS * HEAD_DIM), bf16),
            pltpu.VMEM((members, 3, HEADS, block, HEAD_DIM), bf16),
            pltpu.VMEM((HEADS, block, HEAD_DIM), bf16),
            pltpu.VMEM((HEADS, block, HEAD_DIM), bf16),
            pltpu.VMEM((seq_len, seq_len), bf16),
            dma((2 * others,)),
            dma((2 * others,)),
            dma((beside,)),
            dma((beside,)),
            dma((beside,)),
            dma((beside,)),
            dma((others,)),
            dma((others,)),
            dma((beside,)),
            dma((beside,)),
            dma((beside,)),
            dma((beside,)),
            dma((members * HEADS,)),
            dma((members * HEADS,)),
            dma((others,)),
            dma((others,)),
            dma((10,)),
        ],
        compiler_params=pltpu.CompilerParams(
            collective_id=0, has_side_effects=True, vmem_limit_bytes=67_043_328
        ),
    )(
        tokens.reshape(block, depth),
        w_query.T,
        w_forward.T,
        w_backward.T,
        w_input.T,
        w_gate.T,
        w_out.T,
        memory_forward.reshape(1, -1),
        memory_backward.reshape(1, -1),
        norm_gain.reshape(1, -1),
    )
    return flat.reshape(1, block, depth)


def layer(mesh, tokens, w_query, *rest):
    members = mesh.shape["sp"] // HEADS
    columns = mesh.shape["dp"] // 2
    if tokens.shape[0] == 1 and w_query.shape[1] % 16 == 0:
        return whole_layer(members, columns, tokens, w_query, *rest)
    return body(tokens, w_query, *rest)


def solution(mesh):
    return jax.shard_map(
        functools.partial(layer, mesh),
        mesh=mesh,
        in_specs=(
            P("dp", "sp", None),
            P(None, ("sp", "dp")),
            P(None, ("sp", "dp")),
            P(None, ("sp", "dp")),
            P(None, ("sp", "dp")),
            P(None, ("sp", "dp")),
            P(None, ("sp", "dp")),
            P(),
            P(),
            P(),
        ),
        out_specs=P("dp", "sp", None),
        check_vma=False,
    )
```

```python
import functools

import jax
import jax.numpy as jnp
from jax import lax
from jax.experimental import pallas as pl
from jax.experimental.pallas import tpu as pltpu
from jax.sharding import PartitionSpec as P

HEADS = 4
HEAD_DIM = 128
BLOCK = 64


norm_eps = 1e-06
highest = lax.Precision.HIGHEST


def as_sent(array):
    return jax.tree.map(lambda a: a.astype(jnp.bfloat16) if a.dtype == jnp.float32 else a, array)


def gathered_then(share, axis, dim, apply):
    everything = lax.all_gather(share, axis, axis=dim, tiled=True)
    return apply(everything, jnp.int32(0))


def log_forget(projected, memory, seq_len):
    slack_value = memory / seq_len
    return jnp.logaddexp(
        jnp.log1p(-slack_value),
        jnp.log(slack_value) + jax.nn.log_sigmoid(projected.astype(jnp.float32)),
    )


def sweep(queries, log_decay, values):
    seq_len, key_width = queries.shape
    blocks = seq_len // BLOCK
    input_keys = -jnp.expm1(log_decay)
    lower_mask = jnp.tril(jnp.ones((BLOCK, BLOCK), dtype=bool))[:, :, None]

    def advance(carry_state, inputs):
        query_part, decay_part, key_part, value_part = inputs
        running = jnp.cumsum(decay_part, axis=0)
        from_state = jnp.dot(query_part * jnp.exp(running), carry_state, precision=highest)
        gaps = running[:, None, :] - running[None, :, :]
        decay_table = jnp.where(lower_mask, jnp.exp(jnp.where(lower_mask, gaps, 0.0)), 0.0)
        scores = jnp.sum(query_part[:, None, :] * key_part[None, :, :] * decay_table, axis=2)
        inside = jnp.dot(scores, value_part, precision=highest)
        final_sum = running[-1]
        weighted = key_part * jnp.exp(final_sum[None, :] - running)
        carry_state = jnp.exp(final_sum)[:, None] * carry_state + jnp.dot(
            weighted.T, value_part, precision=highest
        )
        return (carry_state, from_state + inside)

    def blocked(array):
        return array.reshape(blocks, BLOCK, array.shape[1])

    zero_state = jnp.zeros((key_width, values.shape[1]), jnp.float32)
    _, readings = lax.scan(
        advance,
        zero_state,
        (blocked(queries), blocked(log_decay), blocked(input_keys), blocked(values)),
    )
    return readings.reshape(seq_len, values.shape[1])


def both_ways(queries, log_ahead, log_behind, values):
    forward_read = sweep(queries, log_ahead, values)
    behind = sweep(jnp.flip(queries, 0), jnp.flip(log_behind, 0), jnp.flip(values, 0))
    return forward_read + jnp.flip(behind, 0)


def body(
    tokens,
    w_query,
    w_forward,
    w_backward,
    w_input,
    w_gate,
    w_out,
    memory_forward,
    memory_backward,
    norm_gain,
):
    seq_count, tok_count, model_width = tokens.shape
    row_count = seq_count * tok_count
    flat_tokens = tokens.reshape(row_count, model_width)
    group_count = lax.axis_size("sp")
    per_head_groups = group_count // HEADS
    block_width = HEAD_DIM // per_head_groups
    head_index = lax.axis_index("sp") // per_head_groups
    full_query, full_forward, full_backward, full_input, full_gate = (
        lax.all_gather(w_query, ("sp", "dp"), axis=1, tiled=True),
        lax.all_gather(w_forward, ("sp", "dp"), axis=1, tiled=True),
        lax.all_gather(w_backward, ("sp", "dp"), axis=1, tiled=True),
        lax.all_gather(w_input, ("sp", "dp"), axis=1, tiled=True),
        lax.all_gather(w_gate, ("sp", "dp"), axis=1, tiled=True),
    )

    def project(weight):
        return jnp.dot(flat_tokens, weight, preferred_element_type=jnp.float32).astype(jnp.bfloat16)

    def by_head(projected):
        shaped = projected.reshape(row_count, HEADS, 1, HEAD_DIM)
        spread_out = jnp.broadcast_to(shaped, (row_count, HEADS, per_head_groups, HEAD_DIM))
        return spread_out.reshape(row_count, group_count, HEAD_DIM)

    def by_group(projected):
        return projected.reshape(row_count, group_count, block_width)

    query_heads, ahead_heads, behind_heads, value_heads = (
        lax.all_to_all(
            as_sent(by_head(project(full_query))), "sp", split_axis=1, concat_axis=0, tiled=True
        ),
        lax.all_to_all(
            as_sent(by_head(project(full_forward))), "sp", split_axis=1, concat_axis=0, tiled=True
        ),
        lax.all_to_all(
            as_sent(by_head(project(full_backward))), "sp", split_axis=1, concat_axis=0, tiled=True
        ),
        lax.all_to_all(
            as_sent(by_group(project(full_input))), "sp", split_axis=1, concat_axis=0, tiled=True
        ),
    )
    gate_rows = project(full_gate)
    seq_len = query_heads.shape[0]
    memory_ahead = lax.dynamic_slice_in_dim(memory_forward, head_index * HEAD_DIM, HEAD_DIM)
    memory_behind = lax.dynamic_slice_in_dim(memory_backward, head_index * HEAD_DIM, HEAD_DIM)
    queries = jax.nn.silu(query_heads[:, 0].astype(jnp.float32))
    log_ahead = log_forget(ahead_heads[:, 0], memory_ahead, seq_len)
    log_behind = log_forget(behind_heads[:, 0], memory_behind, seq_len)
    values = value_heads[:, 0].astype(jnp.float32)
    readout = both_ways(queries, log_ahead, log_behind, values).astype(jnp.bfloat16)
    returned = lax.all_to_all(
        readout.reshape(seq_len, 1, block_width), "sp", split_axis=0, concat_axis=1, tiled=True
    )
    readout_rows = returned.reshape(row_count, HEADS, HEAD_DIM).astype(jnp.float32)
    normed = (
        readout_rows
        * lax.rsqrt(jnp.mean(readout_rows * readout_rows, axis=-1, keepdims=True) + norm_eps)
        * norm_gain
    )
    normed = normed.reshape(row_count, HEADS * HEAD_DIM)
    gated_rows = (normed * jax.nn.silu(gate_rows.astype(jnp.float32))).astype(jnp.bfloat16)

    def output_block(weight_piece, first_index):
        return jnp.dot(gated_rows, weight_piece, preferred_element_type=jnp.float32).astype(
            jnp.bfloat16
        )

    mixed_rows = gathered_then(w_out, ("sp", "dp"), 1, output_block)
    return mixed_rows.reshape(seq_count, tok_count, model_width)


GROUPS = ((0, 1), (2,), (3,))
PIECES = 4


def dot_nt(left, right):
    return lax.dot_general(
        left, right, (((1,), (1,)), ((), ())), preferred_element_type=jnp.float32
    )


def layer_kernel(
    members,
    columns,
    tokens,
    w_query,
    w_forward,
    w_backward,
    w_input,
    w_gate,
    w_out,
    memory_forward,
    memory_backward,
    norm_gain,
    mixed,
    small,
    gain,
    query_gate,
    token_all,
    weight_all,
    out_all,
    raw,
    mixed_heads,
    gated_own,
    sum_mask,
    token_send,
    token_recv,
    weight_send,
    weight_recv,
    relay_send,
    relay_recv,
    out_send,
    out_recv,
    plane_send,
    plane_recv,
    back_send,
    back_recv,
    raw_send,
    raw_recv,
    gated_send,
    gated_recv,
    local_sem,
):
    bf16, f32 = jnp.bfloat16, jnp.float32
    block, depth = tokens.shape
    height = block // PIECES
    own_rows = HEADS * block
    sp, dp = lax.axis_index("sp"), lax.axis_index("dp")
    head, member = sp // members, lax.rem(sp, members)
    column, core = dp // 2, lax.rem(dp, 2)
    seq_len = own_rows * members
    heads = (head, head + 1 - 2 * lax.rem(head, 2), lax.rem(head + 2, HEADS), HEADS - 1 - head)

    def turned(index, step, size):
        return lax.rem(index + step, size)

    def device(h, r, x, c):
        return {"sp": h * members + r, "dp": x * 2 + c}

    plane = [(a, b) for a in range(members) for b in range(columns) if (a, b) != (0, 0)]
    plane.sort(key=lambda ab: -((ab[0] != 0) + (ab[1] != 0)))
    last = len(plane)

    def remote(src, dst, send, recv, where):
        return pltpu.make_async_remote_copy(
            src_ref=src,
            dst_ref=dst,
            send_sem=send,
            recv_sem=recv,
            device_id=where,
            device_id_type=pl.DeviceIdType.MESH,
        )

    across = [device(heads[k], member, column, core) for k in range(HEADS)]
    beside = [
        device(head, turned(member, a, members), turned(column, b, columns), core)
        for a, b in plane
    ]
    partner = device(head, member, column, 1 - core)

    weights = (w_forward, w_backward, w_input, w_query, w_gate)
    local = []
    for j, weight in enumerate(weights):
        local.append(pltpu.make_async_copy(weight, weight_all.at[j, member, dp], local_sem.at[j]))
    local.append(pltpu.make_async_copy(tokens, token_all.at[0], local_sem.at[5]))
    local.append(
        pltpu.make_async_copy(w_out, out_all.at[head, member, dp], local_sem.at[6])
    )
    local.append(pltpu.make_async_copy(memory_forward, small.at[0:1], local_sem.at[7]))
    local.append(pltpu.make_async_copy(memory_backward, small.at[1:2], local_sem.at[8]))
    local.append(pltpu.make_async_copy(norm_gain, gain, local_sem.at[9]))
    for copy in [local[5]] + local[:5] + local[6:]:
        copy.start()

    barrier = pltpu.get_barrier_semaphore()
    greeted = across[1:3] + beside + [partner]
    for where in greeted:
        pl.semaphore_signal(barrier, inc=1, device_id=where, device_id_type=pl.DeviceIdType.MESH)
    pl.semaphore_wait(barrier, len(greeted))

    token_copies = []
    local[5].wait()

    def rows_of(k, piece):
        return token_all.at[k, piece * height : (piece + 1) * height]

    def send_tokens(source, slot, where):
        for piece in range(PIECES):
            at = PIECES * (slot - 1) + piece
            copy = remote(
                rows_of(source, piece),
                rows_of(slot, piece),
                token_send.at[at],
                token_recv.at[at],
                where,
            )
            token_copies.append(copy)

    send_tokens(0, 1, across[1])
    send_tokens(0, 2, across[2])
    for copy in token_copies:
        copy.start()

    def weight_block(part, r, x, c):
        return weight_all.at[part, r, x * 2 + c]

    parts = (slice(0, 3), slice(3, 5))
    for copy in local[:5]:
        copy.wait()
    weight_copies = {}
    for p, part in enumerate(parts):
        mine = weight_block(part, member, column, core)
        for i, where in enumerate(beside + [partner]):
            at = 2 * i + p
            copy = remote(mine, mine, weight_send.at[at], weight_recv.at[at], where)
            copy.start()
            weight_copies[i, p] = copy
    local[6].wait()
    out_mine = out_all.at[head, member, dp]
    out_copies = []
    for k in (1, 2):
        copy = remote(out_mine, out_mine, out_send.at[k - 1], out_recv.at[k - 1], across[k])
        copy.start()
        out_copies.append(copy)

    def places(shape, dim, slot):
        row = lax.broadcasted_iota(jnp.int32, shape, dim)
        return (row // block) * (members * block) + lax.rem(row, block) + turned(
            member, slot, members
        ) * block

    for a in range(members):
        for b in range(members):
            shape = (own_rows, own_rows)
            earlier = places(shape, 1, b) <= places(shape, 0, a)
            sum_mask[a * own_rows : (a + 1) * own_rows, b * own_rows : (b + 1) * own_rows] = (
                jnp.where(earlier, 1.0, 0.0).astype(bf16)
            )

    send_tokens(2, 3, across[1])
    for piece in range(PIECES):
        token_copies[PIECES + piece].wait_recv()
        token_copies[2 * PIECES + piece].start()

    relays = {}

    def relay_weights(p):
        for i, (a, b) in enumerate(plane):
            r = turned(member, members - a, members)
            x = turned(column, columns - b, columns)
            landed = weight_block(parts[p], r, x, core)
            weight_copies[i, p].wait_recv()
            at = 2 * i + p
            copy = remote(landed, landed, relay_send.at[at], relay_recv.at[at], partner)
            copy.start()
            relays[i, p] = copy

    def weights_there(p):
        weight_copies[last, p].wait_recv()
        for i in range(last):
            relays[i, p].wait_recv()

    plane_copies = {}
    across_member = device(head, 1 - member, column, core)
    across_column = device(head, member, 1 - column, core)

    def send_out(slot, kind):
        owner = 1 - member if kind == 2 else member
        where = (across_member, across_column, across_column, partner)[kind]
        landed = out_all.at[heads[slot], owner, dp]
        at = HEADS * kind + slot
        copy = remote(landed, landed, plane_send.at[at], plane_recv.at[at], where)
        copy.start()
        plane_copies[kind, slot] = copy

    def spread_out(slot):
        for kind in (0, 1, 3):
            send_out(slot, kind)

    def pass_out(slot):
        plane_copies[0, slot].wait_recv()
        send_out(slot, 2)

    spread_out(0)
    relay_weights(0)
    def project(slots, first, count):
        rows = token_all[slots[0] : slots[-1] + 1].reshape(len(slots) * block, depth)
        weight = weight_all[first : first + count].reshape(count * HEAD_DIM, depth)
        return dot_nt(rows, weight).astype(bf16)

    raw_copies = []
    weights_there(0)
    for slots in GROUPS:
        for slot in slots:
            if slot in (1, 3):
                for piece in range(PIECES):
                    token_copies[PIECES * (slot - 1) + piece].wait_recv()
        sent = project(slots, 0, 3)
        for n, slot in enumerate(slots):
            for j in range(3):
                raw[0, j, heads[slot]] = sent[
                    n * block : (n + 1) * block, j * HEAD_DIM : (j + 1) * HEAD_DIM
                ]
        for slot in slots:
            for a in range(1, members):
                at = (a - 1) * HEADS + slot
                copy = remote(
                    raw.at[0, :, heads[slot]],
                    raw.at[members - a, :, heads[slot]],
                    raw_send.at[at],
                    raw_recv.at[at],
                    device(head, turned(member, a, members), column, core),
                )
                copy.start()
                raw_copies.append(copy)
        if slots == GROUPS[0]:
            relay_weights(1)
            out_copies[1].wait_recv()
            landed = out_all.at[heads[2], member, dp]
            copy = remote(landed, landed, out_send.at[2], out_recv.at[2], across[1])
            copy.start()
            out_copies.append(copy)
            out_copies[0].wait_recv()
            spread_out(1)
            spread_out(2)
    out_copies[2].wait_recv()
    spread_out(3)
    weights_there(1)
    sent = project((0, 1, 2, 3), 3, 2)
    for slot in range(HEADS):
        for j in range(2):
            query_gate[j, heads[slot]] = sent[
                slot * block : (slot + 1) * block, j * HEAD_DIM : (j + 1) * HEAD_DIM
            ]
    for slot in range(3):
        pass_out(slot)

    gate = query_gate[1].reshape(own_rows, HEAD_DIM).astype(f32)
    query = query_gate[0].reshape(own_rows, HEAD_DIM).astype(f32)
    queries = query * jax.nn.sigmoid(query)
    gate = gate * jax.nn.sigmoid(gate)
    for copy in local[7:]:
        copy.wait()

    channels = pl.ds(pl.multiple_of(head * HEAD_DIM, HEAD_DIM), HEAD_DIM)

    def keys_of(a, j):
        slack_value = small[j : j + 1, channels] / seq_len
        projected = raw[a, j].reshape(own_rows, HEAD_DIM).astype(f32)
        key = slack_value * jax.nn.sigmoid(-projected)
        return key, jnp.log1p(-key)

    made = [(keys_of(0, 0), keys_of(0, 1))]
    pass_out(3)
    for copy in raw_copies:
        copy.wait_recv()
    for a in range(1, members):
        made.append((keys_of(a, 0), keys_of(a, 1)))

    def joined(way, item):
        return jnp.concatenate([one[way][item] for one in made], axis=0)

    key_ahead, log_ahead = joined(0, 0), joined(0, 1)
    key_behind, log_behind = joined(1, 0), joined(1, 1)
    values = raw[:, 2].reshape(seq_len, HEAD_DIM)
    logs = jnp.concatenate([log_ahead, log_behind], axis=1)
    coarse = logs.astype(bf16)
    fine = (logs - coarse.astype(f32)).astype(bf16)
    sums = jnp.dot(
        sum_mask[...], jnp.concatenate([coarse, fine], axis=1), preferred_element_type=f32
    )
    sums = sums[:, : 2 * HEAD_DIM] + sums[:, 2 * HEAD_DIM :]
    ahead = sums[:, :HEAD_DIM]
    behind = sums[:, HEAD_DIM:] - log_behind
    query_ahead = (queries * jnp.exp(ahead[:own_rows])).astype(bf16)
    query_behind = (queries * jnp.exp(-behind[:own_rows])).astype(bf16)
    key_ahead = (key_ahead * jnp.exp(-ahead)).astype(bf16)
    key_behind = (key_behind * jnp.exp(behind)).astype(bf16)

    readout = jnp.zeros((own_rows, HEAD_DIM), f32)
    for b in range(members):
        part = slice(b * own_rows, (b + 1) * own_rows)
        shape = (own_rows, own_rows)
        there, here = places(shape, 1, b), places(shape, 0, 0)
        scores = jnp.where(there <= here, dot_nt(query_ahead, key_ahead[part]), 0.0) + jnp.where(
            there >= here, dot_nt(query_behind, key_behind[part]), 0.0
        )
        readout = readout + jnp.dot(
            scores.astype(bf16), values[part], preferred_element_type=f32
        )
    readout = readout.astype(bf16).astype(f32)
    square = jnp.mean(readout * readout, axis=-1, keepdims=True)
    gated = (readout * lax.rsqrt(square + norm_eps) * gain[...] * gate).astype(bf16)
    gated_own[...] = gated.reshape(HEADS, block, HEAD_DIM)

    gated_copies = []
    for k in range(1, HEADS):
        copy = remote(
            gated_own.at[heads[k]],
            mixed_heads.at[head],
            gated_send.at[k - 1],
            gated_recv.at[k - 1],
            across[k],
        )
        copy.start()
        gated_copies.append(copy)
    mixed_heads[head] = gated_own[head]

    back_copies = []
    for kind, (r, x) in enumerate(
        ((1 - member, column), (member, 1 - column), (1 - member, 1 - column))
    ):
        for slot in range(HEADS):
            if kind > 0:
                plane_copies[kind, slot].wait_recv()
        landed = out_all.at[:, r, x * 2 + core]
        copy = remote(landed, landed, back_send.at[kind], back_recv.at[kind], partner)
        copy.start()
        back_copies.append(copy)
    for slot in range(HEADS):
        plane_copies[3, slot].wait_recv()
    for copy in back_copies:
        copy.wait_recv()
    total = jnp.zeros((block, depth), f32)
    for k in range(HEADS):
        if k > 0:
            gated_copies[k - 1].wait_recv()
        lanes = pl.ds(pl.multiple_of(heads[k] * HEAD_DIM, HEAD_DIM), HEAD_DIM)
        weight = out_all[:, :, :, :, lanes].reshape(depth, HEAD_DIM)
        total = total + dot_nt(mixed_heads[heads[k]], weight)
    mixed[...] = total.astype(bf16)

    for copy in token_copies + out_copies + back_copies + raw_copies + gated_copies:
        copy.wait_send()
    for copies in (weight_copies, relays, plane_copies):
        for copy in copies.values():
            copy.wait_send()


def whole_layer(
    members,
    columns,
    tokens,
    w_query,
    w_forward,
    w_backward,
    w_input,
    w_gate,
    w_out,
    memory_forward,
    memory_backward,
    norm_gain,
):
    _, block, depth = tokens.shape
    width = w_query.shape[1]
    out_width = w_out.shape[1]
    own_rows = HEADS * block
    seq_len = own_rows * members
    others = HEADS - 1
    beside = members * columns
    bf16 = jnp.bfloat16
    dma = pltpu.SemaphoreType.DMA
    hbm = pl.BlockSpec(memory_space=pltpu.HBM)
    vmem = pl.BlockSpec(memory_space=pltpu.VMEM)
    flat = pl.pallas_call(
        functools.partial(layer_kernel, members, columns),
        out_shape=jax.ShapeDtypeStruct((block, depth), bf16),
        in_specs=[hbm] * 10,
        out_specs=vmem,
        scratch_shapes=[
            pltpu.VMEM((2, HEADS * HEAD_DIM), jnp.float32),
            pltpu.VMEM((1, HEAD_DIM), jnp.float32),
            pltpu.VMEM((2, HEADS, block, HEAD_DIM), bf16),
            pltpu.VMEM((HEADS, block, depth), bf16),
            pltpu.VMEM((5, members, 2 * columns, width, depth), bf16),
            pltpu.VMEM((HEADS, members, 2 * columns, out_width, HEADS * HEAD_DIM), bf16),
            pltpu.VMEM((members, 3, HEADS, block, HEAD_DIM), bf16),
            pltpu.VMEM((HEADS, block, HEAD_DIM), bf16),
            pltpu.VMEM((HEADS, block, HEAD_DIM), bf16),
            pltpu.VMEM((seq_len, seq_len), bf16),
            dma((PIECES * others,)),
            dma((PIECES * others,)),
            dma((2 * beside,)),
            dma((2 * beside,)),
            dma((2 * beside,)),
            dma((2 * beside,)),
            dma((others,)),
            dma((others,)),
            dma((HEADS * beside,)),
            dma((HEADS * beside,)),
            dma((beside,)),
            dma((beside,)),
            dma((members * HEADS,)),
            dma((members * HEADS,)),
            dma((others,)),
            dma((others,)),
            dma((10,)),
        ],
        compiler_params=pltpu.CompilerParams(
            collective_id=0, has_side_effects=True, vmem_limit_bytes=67_043_328
        ),
    )(
        tokens.reshape(block, depth),
        w_query.T,
        w_forward.T,
        w_backward.T,
        w_input.T,
        w_gate.T,
        w_out.T,
        memory_forward.reshape(1, -1),
        memory_backward.reshape(1, -1),
        norm_gain.reshape(1, -1),
    )
    return flat.reshape(1, block, depth)


def layer(mesh, tokens, w_query, *rest):
    members = mesh.shape["sp"] // HEADS
    columns = mesh.shape["dp"] // 2
    fits = members == 2 and columns == 2 and tokens.shape[0] == 1
    if fits and w_query.shape[1] % 16 == 0:
        return whole_layer(members, columns, tokens, w_query, *rest)
    return body(tokens, w_query, *rest)


def solution(mesh):
    return jax.shard_map(
        functools.partial(layer, mesh),
        mesh=mesh,
        in_specs=(
            P("dp", "sp", None),
            P(None, ("sp", "dp")),
            P(None, ("sp", "dp")),
            P(None, ("sp", "dp")),
            P(None, ("sp", "dp")),
            P(None, ("sp", "dp")),
            P(None, ("sp", "dp")),
            P(),
            P(),
            P(),
        ),
        out_specs=P("dp", "sp", None),
        check_vma=False,
    )
```

```python
import functools

import jax
import jax.numpy as jnp
from jax import lax
from jax.experimental import pallas as pl
from jax.experimental.pallas import tpu as pltpu
from jax.sharding import PartitionSpec as P

HEADS = 4
HEAD_DIM = 128
BLOCK = 64


norm_eps = 1e-06
highest = lax.Precision.HIGHEST


def as_sent(array):
    return jax.tree.map(lambda a: a.astype(jnp.bfloat16) if a.dtype == jnp.float32 else a, array)


def gathered_then(share, axis, dim, apply):
    everything = lax.all_gather(share, axis, axis=dim, tiled=True)
    return apply(everything, jnp.int32(0))


def log_forget(projected, memory, seq_len):
    slack_value = memory / seq_len
    return jnp.logaddexp(
        jnp.log1p(-slack_value),
        jnp.log(slack_value) + jax.nn.log_sigmoid(projected.astype(jnp.float32)),
    )


def sweep(queries, log_decay, values):
    seq_len, key_width = queries.shape
    blocks = seq_len // BLOCK
    input_keys = -jnp.expm1(log_decay)
    lower_mask = jnp.tril(jnp.ones((BLOCK, BLOCK), dtype=bool))[:, :, None]

    def advance(carry_state, inputs):
        query_part, decay_part, key_part, value_part = inputs
        running = jnp.cumsum(decay_part, axis=0)
        from_state = jnp.dot(query_part * jnp.exp(running), carry_state, precision=highest)
        gaps = running[:, None, :] - running[None, :, :]
        decay_table = jnp.where(lower_mask, jnp.exp(jnp.where(lower_mask, gaps, 0.0)), 0.0)
        scores = jnp.sum(query_part[:, None, :] * key_part[None, :, :] * decay_table, axis=2)
        inside = jnp.dot(scores, value_part, precision=highest)
        final_sum = running[-1]
        weighted = key_part * jnp.exp(final_sum[None, :] - running)
        carry_state = jnp.exp(final_sum)[:, None] * carry_state + jnp.dot(
            weighted.T, value_part, precision=highest
        )
        return (carry_state, from_state + inside)

    def blocked(array):
        return array.reshape(blocks, BLOCK, array.shape[1])

    zero_state = jnp.zeros((key_width, values.shape[1]), jnp.float32)
    _, readings = lax.scan(
        advance,
        zero_state,
        (blocked(queries), blocked(log_decay), blocked(input_keys), blocked(values)),
    )
    return readings.reshape(seq_len, values.shape[1])


def both_ways(queries, log_ahead, log_behind, values):
    forward_read = sweep(queries, log_ahead, values)
    behind = sweep(jnp.flip(queries, 0), jnp.flip(log_behind, 0), jnp.flip(values, 0))
    return forward_read + jnp.flip(behind, 0)


def body(
    tokens,
    w_query,
    w_forward,
    w_backward,
    w_input,
    w_gate,
    w_out,
    memory_forward,
    memory_backward,
    norm_gain,
):
    seq_count, tok_count, model_width = tokens.shape
    row_count = seq_count * tok_count
    flat_tokens = tokens.reshape(row_count, model_width)
    group_count = lax.axis_size("sp")
    per_head_groups = group_count // HEADS
    block_width = HEAD_DIM // per_head_groups
    head_index = lax.axis_index("sp") // per_head_groups
    full_query, full_forward, full_backward, full_input, full_gate = (
        lax.all_gather(w_query, ("sp", "dp"), axis=1, tiled=True),
        lax.all_gather(w_forward, ("sp", "dp"), axis=1, tiled=True),
        lax.all_gather(w_backward, ("sp", "dp"), axis=1, tiled=True),
        lax.all_gather(w_input, ("sp", "dp"), axis=1, tiled=True),
        lax.all_gather(w_gate, ("sp", "dp"), axis=1, tiled=True),
    )

    def project(weight):
        return jnp.dot(flat_tokens, weight, preferred_element_type=jnp.float32).astype(jnp.bfloat16)

    def by_head(projected):
        shaped = projected.reshape(row_count, HEADS, 1, HEAD_DIM)
        spread_out = jnp.broadcast_to(shaped, (row_count, HEADS, per_head_groups, HEAD_DIM))
        return spread_out.reshape(row_count, group_count, HEAD_DIM)

    def by_group(projected):
        return projected.reshape(row_count, group_count, block_width)

    query_heads, ahead_heads, behind_heads, value_heads = (
        lax.all_to_all(
            as_sent(by_head(project(full_query))), "sp", split_axis=1, concat_axis=0, tiled=True
        ),
        lax.all_to_all(
            as_sent(by_head(project(full_forward))), "sp", split_axis=1, concat_axis=0, tiled=True
        ),
        lax.all_to_all(
            as_sent(by_head(project(full_backward))), "sp", split_axis=1, concat_axis=0, tiled=True
        ),
        lax.all_to_all(
            as_sent(by_group(project(full_input))), "sp", split_axis=1, concat_axis=0, tiled=True
        ),
    )
    gate_rows = project(full_gate)
    seq_len = query_heads.shape[0]
    memory_ahead = lax.dynamic_slice_in_dim(memory_forward, head_index * HEAD_DIM, HEAD_DIM)
    memory_behind = lax.dynamic_slice_in_dim(memory_backward, head_index * HEAD_DIM, HEAD_DIM)
    queries = jax.nn.silu(query_heads[:, 0].astype(jnp.float32))
    log_ahead = log_forget(ahead_heads[:, 0], memory_ahead, seq_len)
    log_behind = log_forget(behind_heads[:, 0], memory_behind, seq_len)
    values = value_heads[:, 0].astype(jnp.float32)
    readout = both_ways(queries, log_ahead, log_behind, values).astype(jnp.bfloat16)
    returned = lax.all_to_all(
        readout.reshape(seq_len, 1, block_width), "sp", split_axis=0, concat_axis=1, tiled=True
    )
    readout_rows = returned.reshape(row_count, HEADS, HEAD_DIM).astype(jnp.float32)
    normed = (
        readout_rows
        * lax.rsqrt(jnp.mean(readout_rows * readout_rows, axis=-1, keepdims=True) + norm_eps)
        * norm_gain
    )
    normed = normed.reshape(row_count, HEADS * HEAD_DIM)
    gated_rows = (normed * jax.nn.silu(gate_rows.astype(jnp.float32))).astype(jnp.bfloat16)

    def output_block(weight_piece, first_index):
        return jnp.dot(gated_rows, weight_piece, preferred_element_type=jnp.float32).astype(
            jnp.bfloat16
        )

    mixed_rows = gathered_then(w_out, ("sp", "dp"), 1, output_block)
    return mixed_rows.reshape(seq_count, tok_count, model_width)


GROUPS = ((0, 1, 2), (3,))
PIECES = 2


def dot_nt(left, right):
    return lax.dot_general(
        left, right, (((1,), (1,)), ((), ())), preferred_element_type=jnp.float32
    )


def layer_kernel(
    members,
    columns,
    tokens,
    w_query,
    w_forward,
    w_backward,
    w_input,
    w_gate,
    w_out,
    memory_forward,
    memory_backward,
    norm_gain,
    mixed,
    small,
    gain,
    query_gate,
    token_all,
    weight_all,
    out_all,
    raw,
    mixed_heads,
    gated_own,
    sum_mask,
    token_send,
    token_recv,
    weight_send,
    weight_recv,
    relay_send,
    relay_recv,
    out_send,
    out_recv,
    plane_send,
    plane_recv,
    back_send,
    back_recv,
    raw_send,
    raw_recv,
    gated_send,
    gated_recv,
    local_sem,
):
    bf16, f32 = jnp.bfloat16, jnp.float32
    block, depth = tokens.shape
    height = block // PIECES
    own_rows = HEADS * block
    sp, dp = lax.axis_index("sp"), lax.axis_index("dp")
    head, member = sp // members, lax.rem(sp, members)
    column, core = dp // 2, lax.rem(dp, 2)
    seq_len = own_rows * members
    heads = (head, head + 1 - 2 * lax.rem(head, 2), lax.rem(head + 2, HEADS), HEADS - 1 - head)

    def turned(index, step, size):
        return lax.rem(index + step, size)

    def device(h, r, x, c):
        return {"sp": h * members + r, "dp": x * 2 + c}

    plane = [(a, b) for a in range(members) for b in range(columns) if (a, b) != (0, 0)]
    plane.sort(key=lambda ab: -((ab[0] != 0) + (ab[1] != 0)))
    last = len(plane)

    def remote(src, dst, send, recv, where):
        return pltpu.make_async_remote_copy(
            src_ref=src,
            dst_ref=dst,
            send_sem=send,
            recv_sem=recv,
            device_id=where,
            device_id_type=pl.DeviceIdType.MESH,
        )

    across = [device(heads[k], member, column, core) for k in range(HEADS)]
    beside = [
        device(head, turned(member, a, members), turned(column, b, columns), core)
        for a, b in plane
    ]
    partner = device(head, member, column, 1 - core)

    weights = (w_forward, w_backward, w_input, w_query, w_gate)
    local = []
    for j, weight in enumerate(weights):
        local.append(pltpu.make_async_copy(weight, weight_all.at[j, member, dp], local_sem.at[j]))
    local.append(pltpu.make_async_copy(tokens, token_all.at[0], local_sem.at[5]))
    local.append(
        pltpu.make_async_copy(w_out, out_all.at[head, member, dp], local_sem.at[6])
    )
    local.append(pltpu.make_async_copy(memory_forward, small.at[0:1], local_sem.at[7]))
    local.append(pltpu.make_async_copy(memory_backward, small.at[1:2], local_sem.at[8]))
    local.append(pltpu.make_async_copy(norm_gain, gain, local_sem.at[9]))
    for copy in [local[5]] + local[:5] + local[6:]:
        copy.start()

    barrier = pltpu.get_barrier_semaphore()
    greeted = across[1:3] + beside + [partner]
    for where in greeted:
        pl.semaphore_signal(barrier, inc=1, device_id=where, device_id_type=pl.DeviceIdType.MESH)
    pl.semaphore_wait(barrier, len(greeted))

    token_copies = []
    local[5].wait()

    def rows_of(k, piece):
        return token_all.at[k, piece * height : (piece + 1) * height]

    def send_tokens(source, slot, where):
        for piece in range(PIECES):
            at = PIECES * (slot - 1) + piece
            copy = remote(
                rows_of(source, piece),
                rows_of(slot, piece),
                token_send.at[at],
                token_recv.at[at],
                where,
            )
            token_copies.append(copy)

    send_tokens(0, 1, across[1])
    send_tokens(0, 2, across[2])
    for copy in token_copies:
        copy.start()

    def weight_block(part, r, x, c):
        return weight_all.at[part, r, x * 2 + c]

    parts = (slice(0, 3), slice(3, 5))
    for copy in local[:5]:
        copy.wait()
    weight_copies = {}
    for p, part in enumerate(parts):
        mine = weight_block(part, member, column, core)
        for i, where in enumerate(beside + [partner]):
            at = 2 * i + p
            copy = remote(mine, mine, weight_send.at[at], weight_recv.at[at], where)
            copy.start()
            weight_copies[i, p] = copy
    local[6].wait()
    out_mine = out_all.at[head, member, dp]
    out_copies = []
    for k in (1, 2):
        copy = remote(out_mine, out_mine, out_send.at[k - 1], out_recv.at[k - 1], across[k])
        copy.start()
        out_copies.append(copy)

    def places(shape, dim, slot):
        row = lax.broadcasted_iota(jnp.int32, shape, dim)
        return (row // block) * (members * block) + lax.rem(row, block) + turned(
            member, slot, members
        ) * block

    for a in range(members):
        for b in range(members):
            shape = (own_rows, own_rows)
            earlier = places(shape, 1, b) <= places(shape, 0, a)
            sum_mask[a * own_rows : (a + 1) * own_rows, b * own_rows : (b + 1) * own_rows] = (
                jnp.where(earlier, 1.0, 0.0).astype(bf16)
            )

    send_tokens(2, 3, across[1])
    for piece in range(PIECES):
        token_copies[PIECES + piece].wait_recv()
        token_copies[2 * PIECES + piece].start()

    relays = {}

    def relay_weights(p):
        for i, (a, b) in enumerate(plane):
            r = turned(member, members - a, members)
            x = turned(column, columns - b, columns)
            landed = weight_block(parts[p], r, x, core)
            weight_copies[i, p].wait_recv()
            at = 2 * i + p
            copy = remote(landed, landed, relay_send.at[at], relay_recv.at[at], partner)
            copy.start()
            relays[i, p] = copy

    def weights_there(p):
        weight_copies[last, p].wait_recv()
        for i in range(last):
            relays[i, p].wait_recv()

    plane_copies = {}
    across_member = device(head, 1 - member, column, core)
    across_column = device(head, member, 1 - column, core)

    def send_out(slot, kind):
        owner = 1 - member if kind == 2 else member
        where = (across_member, across_column, across_column, partner)[kind]
        landed = out_all.at[heads[slot], owner, dp]
        at = HEADS * kind + slot
        copy = remote(landed, landed, plane_send.at[at], plane_recv.at[at], where)
        copy.start()
        plane_copies[kind, slot] = copy

    def spread_out(slot):
        for kind in (0, 1, 3):
            send_out(slot, kind)

    def pass_out(slot):
        plane_copies[0, slot].wait_recv()
        send_out(slot, 2)

    spread_out(0)
    relay_weights(0)
    def project(slots, first, count):
        rows = token_all[slots[0] : slots[-1] + 1].reshape(len(slots) * block, depth)
        weight = weight_all[first : first + count].reshape(count * HEAD_DIM, depth)
        return dot_nt(rows, weight).astype(bf16)

    raw_copies = []
    weights_there(0)
    for slots in GROUPS:
        for slot in slots:
            if slot in (1, 3):
                for piece in range(PIECES):
                    token_copies[PIECES * (slot - 1) + piece].wait_recv()
        sent = project(slots, 0, 3)
        for n, slot in enumerate(slots):
            for j in range(3):
                raw[0, j, heads[slot]] = sent[
                    n * block : (n + 1) * block, j * HEAD_DIM : (j + 1) * HEAD_DIM
                ]
        for slot in slots:
            for a in range(1, members):
                at = (a - 1) * HEADS + slot
                copy = remote(
                    raw.at[0, :, heads[slot]],
                    raw.at[members - a, :, heads[slot]],
                    raw_send.at[at],
                    raw_recv.at[at],
                    device(head, turned(member, a, members), column, core),
                )
                copy.start()
                raw_copies.append(copy)
        if slots == GROUPS[0]:
            relay_weights(1)
            out_copies[1].wait_recv()
            landed = out_all.at[heads[2], member, dp]
            copy = remote(landed, landed, out_send.at[2], out_recv.at[2], across[1])
            copy.start()
            out_copies.append(copy)
            out_copies[0].wait_recv()
            spread_out(1)
            spread_out(2)
    out_copies[2].wait_recv()
    spread_out(3)
    weights_there(1)
    sent = project((0, 1, 2, 3), 3, 2)
    for slot in range(HEADS):
        for j in range(2):
            query_gate[j, heads[slot]] = sent[
                slot * block : (slot + 1) * block, j * HEAD_DIM : (j + 1) * HEAD_DIM
            ]
    for slot in range(3):
        pass_out(slot)

    gate = query_gate[1].reshape(own_rows, HEAD_DIM).astype(f32)
    query = query_gate[0].reshape(own_rows, HEAD_DIM).astype(f32)
    queries = query * jax.nn.sigmoid(query)
    gate = gate * jax.nn.sigmoid(gate)
    for copy in local[7:]:
        copy.wait()

    channels = pl.ds(pl.multiple_of(head * HEAD_DIM, HEAD_DIM), HEAD_DIM)

    def keys_of(a, j):
        slack_value = small[j : j + 1, channels] / seq_len
        projected = raw[a, j].reshape(own_rows, HEAD_DIM).astype(f32)
        key = slack_value * jax.nn.sigmoid(-projected)
        return key, jnp.log1p(-key)

    made = [(keys_of(0, 0), keys_of(0, 1))]
    pass_out(3)
    for copy in raw_copies:
        copy.wait_recv()
    for a in range(1, members):
        made.append((keys_of(a, 0), keys_of(a, 1)))

    def joined(way, item):
        return jnp.concatenate([one[way][item] for one in made], axis=0)

    key_ahead, log_ahead = joined(0, 0), joined(0, 1)
    key_behind, log_behind = joined(1, 0), joined(1, 1)
    values = raw[:, 2].reshape(seq_len, HEAD_DIM)
    logs = jnp.concatenate([log_ahead, log_behind], axis=1)
    coarse = logs.astype(bf16)
    fine = (logs - coarse.astype(f32)).astype(bf16)
    sums = jnp.dot(
        sum_mask[...], jnp.concatenate([coarse, fine], axis=1), preferred_element_type=f32
    )
    sums = sums[:, : 2 * HEAD_DIM] + sums[:, 2 * HEAD_DIM :]
    ahead = sums[:, :HEAD_DIM]
    behind = sums[:, HEAD_DIM:] - log_behind
    query_ahead = (queries * jnp.exp(ahead[:own_rows])).astype(bf16)
    query_behind = (queries * jnp.exp(-behind[:own_rows])).astype(bf16)
    key_ahead = (key_ahead * jnp.exp(-ahead)).astype(bf16)
    key_behind = (key_behind * jnp.exp(behind)).astype(bf16)

    readout = jnp.zeros((own_rows, HEAD_DIM), f32)
    for b in range(members):
        part = slice(b * own_rows, (b + 1) * own_rows)
        shape = (own_rows, own_rows)
        there, here = places(shape, 1, b), places(shape, 0, 0)
        scores = jnp.where(there <= here, dot_nt(query_ahead, key_ahead[part]), 0.0) + jnp.where(
            there >= here, dot_nt(query_behind, key_behind[part]), 0.0
        )
        readout = readout + jnp.dot(
            scores.astype(bf16), values[part], preferred_element_type=f32
        )
    readout = readout.astype(bf16).astype(f32)
    square = jnp.mean(readout * readout, axis=-1, keepdims=True)
    gated = (readout * lax.rsqrt(square + norm_eps) * gain[...] * gate).astype(bf16)
    gated_own[...] = gated.reshape(HEADS, block, HEAD_DIM)

    gated_copies = []
    for k in range(1, HEADS):
        copy = remote(
            gated_own.at[heads[k]],
            mixed_heads.at[head],
            gated_send.at[k - 1],
            gated_recv.at[k - 1],
            across[k],
        )
        copy.start()
        gated_copies.append(copy)
    mixed_heads[head] = gated_own[head]

    back_copies = []
    for kind, (r, x) in enumerate(
        ((1 - member, column), (member, 1 - column), (1 - member, 1 - column))
    ):
        for slot in range(HEADS):
            if kind > 0:
                plane_copies[kind, slot].wait_recv()
        landed = out_all.at[:, r, x * 2 + core]
        copy = remote(landed, landed, back_send.at[kind], back_recv.at[kind], partner)
        copy.start()
        back_copies.append(copy)
    for slot in range(HEADS):
        plane_copies[3, slot].wait_recv()
    for copy in back_copies:
        copy.wait_recv()
    total = jnp.zeros((block, depth), f32)
    for k in range(HEADS):
        if k > 0:
            gated_copies[k - 1].wait_recv()
        lanes = pl.ds(pl.multiple_of(heads[k] * HEAD_DIM, HEAD_DIM), HEAD_DIM)
        weight = out_all[:, :, :, :, lanes].reshape(depth, HEAD_DIM)
        total = total + dot_nt(mixed_heads[heads[k]], weight)
    mixed[...] = total.astype(bf16)

    for copy in token_copies + out_copies + back_copies + raw_copies + gated_copies:
        copy.wait_send()
    for copies in (weight_copies, relays, plane_copies):
        for copy in copies.values():
            copy.wait_send()


def whole_layer(
    members,
    columns,
    tokens,
    w_query,
    w_forward,
    w_backward,
    w_input,
    w_gate,
    w_out,
    memory_forward,
    memory_backward,
    norm_gain,
):
    _, block, depth = tokens.shape
    width = w_query.shape[1]
    out_width = w_out.shape[1]
    own_rows = HEADS * block
    seq_len = own_rows * members
    others = HEADS - 1
    beside = members * columns
    bf16 = jnp.bfloat16
    dma = pltpu.SemaphoreType.DMA
    hbm = pl.BlockSpec(memory_space=pltpu.HBM)
    vmem = pl.BlockSpec(memory_space=pltpu.VMEM)
    flat = pl.pallas_call(
        functools.partial(layer_kernel, members, columns),
        out_shape=jax.ShapeDtypeStruct((block, depth), bf16),
        in_specs=[hbm] * 10,
        out_specs=vmem,
        scratch_shapes=[
            pltpu.VMEM((2, HEADS * HEAD_DIM), jnp.float32),
            pltpu.VMEM((1, HEAD_DIM), jnp.float32),
            pltpu.VMEM((2, HEADS, block, HEAD_DIM), bf16),
            pltpu.VMEM((HEADS, block, depth), bf16),
            pltpu.VMEM((5, members, 2 * columns, width, depth), bf16),
            pltpu.VMEM((HEADS, members, 2 * columns, out_width, HEADS * HEAD_DIM), bf16),
            pltpu.VMEM((members, 3, HEADS, block, HEAD_DIM), bf16),
            pltpu.VMEM((HEADS, block, HEAD_DIM), bf16),
            pltpu.VMEM((HEADS, block, HEAD_DIM), bf16),
            pltpu.VMEM((seq_len, seq_len), bf16),
            dma((PIECES * others,)),
            dma((PIECES * others,)),
            dma((2 * beside,)),
            dma((2 * beside,)),
            dma((2 * beside,)),
            dma((2 * beside,)),
            dma((others,)),
            dma((others,)),
            dma((HEADS * beside,)),
            dma((HEADS * beside,)),
            dma((beside,)),
            dma((beside,)),
            dma((members * HEADS,)),
            dma((members * HEADS,)),
            dma((others,)),
            dma((others,)),
            dma((10,)),
        ],
        compiler_params=pltpu.CompilerParams(
            collective_id=0, has_side_effects=True, vmem_limit_bytes=67_043_328
        ),
    )(
        tokens.reshape(block, depth),
        w_query.T,
        w_forward.T,
        w_backward.T,
        w_input.T,
        w_gate.T,
        w_out.T,
        memory_forward.reshape(1, -1),
        memory_backward.reshape(1, -1),
        norm_gain.reshape(1, -1),
    )
    return flat.reshape(1, block, depth)


def layer(mesh, tokens, w_query, *rest):
    members = mesh.shape["sp"] // HEADS
    columns = mesh.shape["dp"] // 2
    fits = members == 2 and columns == 2 and tokens.shape[0] == 1
    if fits and w_query.shape[1] % 16 == 0:
        return whole_layer(members, columns, tokens, w_query, *rest)
    return body(tokens, w_query, *rest)


def solution(mesh):
    return jax.shard_map(
        functools.partial(layer, mesh),
        mesh=mesh,
        in_specs=(
            P("dp", "sp", None),
            P(None, ("sp", "dp")),
            P(None, ("sp", "dp")),
            P(None, ("sp", "dp")),
            P(None, ("sp", "dp")),
            P(None, ("sp", "dp")),
            P(None, ("sp", "dp")),
            P(),
            P(),
            P(),
        ),
        out_specs=P("dp", "sp", None),
        check_vma=False,
    )
```
